32 devices in a mesh: grp: 2 (over x), ep: 16 (over z, y, core).
Axes of the slice: x: 2, y: 2, z: 4, core: 2. Of those that a mesh axis runs over, the one named last changes fastest.
Arguments:
- stream: bfloat16 [8192, 2048], P(('grp', 'ep')), parts along dimension 0, may hold values from -6 to 6
- norm_gain: float32 [2048], replicated, may hold values from 0.1 to 1.9
- routing: int32 [8192, 4], P(('grp', 'ep')), parts along dimension 0, may hold values from 0 to 31, all different within a row; in each aligned block of 256 rows (0 to 255, 256 to 511, ...) at most 64 rows name the same one
- gates: float32 [8192, 4], P(('grp', 'ep')), parts along dimension 0, may hold values from 0.1 to 1
- w_gate: bfloat16 [32, 2048, 512], P('ep'), may hold values from -0.125 to 0.125
- w_up: bfloat16 [32, 2048, 512], P('ep'), may hold values from -0.125 to 0.125
- w_down: bfloat16 [32, 512, 2048], P('ep'), may hold values from -0.25 to 0.25
- shared_gate: bfloat16 [2048, 512], replicated, may hold values from -0.125 to 0.125
- shared_up: bfloat16 [2048, 512], replicated, may hold values from -0.125 to 0.125
- shared_down: bfloat16 [512, 2048], replicated, may hold values from -0.25 to 0.25
Outputs:
- mixed: bfloat16 [8192, 2048], P(('grp', 'ep')), parts along dimension 0
The draws below stay inside these ranges and needn't reach their ends.
There are 2 independent parts, one for each index of `grp`. The reference program is written for one: setup_inputs(seed, part) draws one part's arguments, and reference() takes and returns one part's arrays. A program takes and returns all parts, laid end to end along the dimension named above; an argument that names none is the same for every part. Nothing has to cross between parts.
Inputs may be any that keep to these rules, and one draw needn't show every extreme that they name: `routing`: each token names 4 different experts. Among the 256 tokens of one index of ep no expert is named more than 64 times, and on some index an expert is named exactly 64 times.
All inputs are finite; a program needn't handle non-finite values.
Results may differ from the reference program's by a relative error of at most 0.007.
Values may be sent and summed in bfloat16 or wider, within the bound.
A program may use at most 128 MiB of HBM per device.

```python
import math
import jax
import jax.numpy as jnp
import numpy as np
from jax import lax

D = 2048
DE = 512
DS = 512
TOP_K = 4
TOK_DEV = 256
TOKENS = 4096
EXPERTS = 32
CAP = 64
N_EP = 16


def block_scale(stream_key, shape, split, low, high):
    level, own = 1.0, jax.random.fold_in(stream_key, 6)
    for axis_at, blocks in split:
        draws = jnp.exp(jax.random.uniform(jax.random.fold_in(own, axis_at), (blocks,), jnp.float32, low / len(split), high / len(split)))
        level = level * jnp.repeat(draws, shape[axis_at] // blocks).reshape([-1 if axis == axis_at else 1 for axis in range(len(shape))])
    return level


def deal_out(rng, own, number, rows, count, top, most, skew):
    sequence = jax.random.permutation(rng, count)
    packed, ordinary = load_shares(count, rows * top, most, skew, True), load_shares(count, rows * top, most, skew, False)
    places = jnp.arange(count)

    def named(sizes, offset_by):
        used = int((sizes > 0).sum())
        fixed = max(1, used // 4)
        moved = fixed + (places - fixed + offset_by * (used - fixed)) % max(1, count - fixed)
        return jnp.zeros((count,), jnp.int32).at[sequence[jnp.where(places < fixed, places, moved)]].set(jnp.asarray(sizes, jnp.int32))

    sizes = jnp.where(number % 4 == 0, named(packed, number // 4), named(ordinary, number - number // 4 - 1))
    mixed = jax.random.permutation(jax.random.fold_in(own, 3), count)
    donor, sink = mixed[0:count // 2 * 2:2], mixed[1:count // 2 * 2:2]
    slack = jnp.minimum(sizes[donor] - 1, most - sizes[sink]) // 2
    slack = jnp.where((donor == sequence[0]) | (sink == sequence[0]) | (sizes[sink] == 0), 0, jnp.maximum(slack, 0))
    moved = jax.random.randint(jax.random.fold_in(own, 4), (count // 2,), 0, 1 << 20) % (slack + 1)
    sizes = sizes.at[donor].add(-moved).at[sink].add(moved)
    members = jnp.searchsorted(jnp.cumsum(sizes), jnp.arange(rows * top), side="right").astype(jnp.int32)
    table = members.reshape(top, rows).T
    table = table[jax.random.permutation(jax.random.fold_in(own, 1), rows)]
    offset_by = jax.random.randint(jax.random.fold_in(own, 2), (rows, 1), 0, top)
    return jnp.take_along_axis(table, (jnp.arange(top)[None, :] + offset_by) % top, axis=1)


def load_shares(number_of, total, limit, slope, full):
    weights = [(1 << 20) // math.isqrt(standing ** slope) + 1 for standing in range(1, number_of + 1)]
    largest = limit if full else min(limit, max(-(-total // number_of), total * weights[0] // sum(weights)))
    least = 1 if total - largest >= number_of - 1 else 0
    counts, surplus = [largest] + [least] * (number_of - 1), total - largest - least * (number_of - 1)
    while surplus > 0:
        movable = [i for i in range(1, number_of) if counts[i] < largest] or [i for i in range(1, number_of) if counts[i] < limit]
        pool, left = sum([weights[i] for i in movable]), surplus
        for i in movable:
            extra = min(limit - counts[i], max(1, left * weights[i] // pool), surplus)
            counts[i] = counts[i] + extra
            surplus = surplus - extra
    return np.array(counts)


def gaussian(own_key, shape, spread, limit, pieces=(), kind=jnp.bfloat16):
    level = block_scale(own_key, shape, pieces, -0.22, 0.18) if pieces else 1.0
    entries = jax.random.normal(own_key, shape, jnp.float32) * spread * level
    return jnp.minimum(jnp.maximum(entries, -limit), limit).astype(kind)


def setup_inputs(seed: int = 0, part: int = 0) -> dict:
    streams_of = jax.random.split(jax.random.key(seed), 11)
    own_keys = jax.random.split(jax.random.fold_in(streams_of[10], part), 11)
    stream = gaussian(own_keys[0], (TOKENS, D), 1.0, 6.0, ((0, 16),))
    norm_gain = jnp.clip(1.0 + 0.18 * jax.random.normal(streams_of[1], (D,), jnp.float32), 0.1, 1.9)
    routing_keys = jax.random.split(jax.random.fold_in(own_keys[2], 1), TOKENS // TOK_DEV)
    routing_turns = jax.random.permutation(jax.random.fold_in(own_keys[2], 3), TOKENS // TOK_DEV)
    routing = jax.vmap(lambda own, number: deal_out(jax.random.fold_in(own_keys[2], 2), own, number, TOK_DEV, EXPERTS, TOP_K, CAP, 2))(routing_keys, routing_turns).reshape((TOKENS, TOP_K))
    gates = jnp.clip(0.1 + 0.9 * jax.random.uniform(own_keys[3], (TOKENS, TOP_K), jnp.float32) ** block_scale(own_keys[3], (TOKENS, TOP_K), ((0, 16),), -0.2, 0.2), 0.1, 1.0)
    w_gate = gaussian(streams_of[4], (EXPERTS, D, DE), D ** -0.5, 0.125, ((0, 16),))
    w_up = gaussian(streams_of[5], (EXPERTS, D, DE), D ** -0.5, 0.125, ((0, 16),))
    w_down = gaussian(streams_of[6], (EXPERTS, DE, D), DE ** -0.5, 0.25, ((0, 16),))
    shared_gate = gaussian(streams_of[7], (D, DS), D ** -0.5, 0.125)
    shared_up = gaussian(streams_of[8], (D, DS), D ** -0.5, 0.125)
    shared_down = gaussian(streams_of[9], (DS, D), DS ** -0.5, 0.25)
    return {"stream": stream, "norm_gain": norm_gain, "routing": routing, "gates": gates, "w_gate": w_gate, "w_up": w_up, "w_down": w_down, "shared_gate": shared_gate, "shared_up": shared_up, "shared_down": shared_down}


def layer_norm(stream, norm_gain):
    widened = stream.astype(jnp.float32)
    row_mean = lax.optimization_barrier(jnp.mean(widened, axis=-1, keepdims=True))
    variance = lax.optimization_barrier(jnp.mean(jnp.square(widened - row_mean), axis=-1, keepdims=True))
    return ((widened - row_mean) * lax.rsqrt(variance + 1e-05) * norm_gain).astype(jnp.bfloat16)

def reference(stream, norm_gain, routing, gates, w_gate, w_up, w_down, shared_gate, shared_up, shared_down):
    normed = layer_norm(stream, norm_gain)
    flat_ids = routing.reshape(-1)
    weights = gates.reshape(-1)
    total_rows = TOKENS * TOP_K
    capacity = N_EP * CAP

    def visit_expert(running, expert):
        chosen = jnp.nonzero(flat_ids == expert, size=capacity, fill_value=total_rows)[0].astype(jnp.int32)
        usable = chosen < total_rows
        clipped = jnp.minimum(chosen, total_rows - 1)
        token_ids = clipped // TOP_K
        gathered = normed[token_ids]
        gate_act = jnp.dot(gathered, w_gate[expert], preferred_element_type=jnp.float32)
        up_act = jnp.dot(gathered, w_up[expert], preferred_element_type=jnp.float32)
        hidden = (jax.nn.silu(gate_act) * up_act).astype(jnp.bfloat16)
        produced = jnp.dot(hidden, w_down[expert], preferred_element_type=jnp.float32).astype(jnp.bfloat16)
        weight_col = jnp.where(usable, weights[clipped], jnp.float32(0.0))
        running = running.at[token_ids].add(produced.astype(jnp.float32) * weight_col[:, None])
        return (running, None)
    start = jnp.zeros((TOKENS, D), jnp.float32)
    routed, _ = lax.scan(visit_expert, start, jnp.arange(EXPERTS, dtype=jnp.int32))
    shared_hidden = (jax.nn.silu(jnp.dot(normed, shared_gate, preferred_element_type=jnp.float32)) * jnp.dot(normed, shared_up, preferred_element_type=jnp.float32)).astype(jnp.bfloat16)
    shared_out = jnp.dot(shared_hidden, shared_down, preferred_element_type=jnp.float32)
    return (routed + shared_out).astype(jnp.bfloat16)
```

```python
import functools
import jax
import jax.numpy as jnp
from jax import lax
from jax.experimental import pallas as pl
from jax.experimental.pallas import tpu as pltpu
from jax.sharding import PartitionSpec as P


def layer_norm(stream, norm_gain):
    widened = stream.astype(jnp.float32)
    row_mean = jnp.mean(widened, axis=-1, keepdims=True)
    variance = jnp.mean(jnp.square(widened - row_mean), axis=-1, keepdims=True)
    return ((widened - row_mean) * lax.rsqrt(variance + 1e-05) * norm_gain).astype(jnp.bfloat16)


def shared_branch(normed, shared_gate, shared_up, shared_down):
    shared_hidden = (
        jax.nn.silu(jnp.dot(normed, shared_gate, preferred_element_type=jnp.float32))
        * jnp.dot(normed, shared_up, preferred_element_type=jnp.float32)
    ).astype(jnp.bfloat16)
    return jnp.dot(shared_hidden, shared_down, preferred_element_type=jnp.float32)


def serve_rows(received, w_gate, w_up, w_down):
    local_count = w_gate.shape[0]
    blocks = received.reshape((-1, local_count) + received.shape[1:])
    gate_act = jnp.einsum("sxcd,xdh->sxch", blocks, w_gate, preferred_element_type=jnp.float32)
    up_act = jnp.einsum("sxcd,xdh->sxch", blocks, w_up, preferred_element_type=jnp.float32)
    hidden = (jax.nn.silu(gate_act) * up_act).astype(jnp.bfloat16)
    produced = jnp.einsum(
        "sxch,xhd->sxcd", hidden, w_down, preferred_element_type=jnp.float32
    ).astype(jnp.bfloat16)
    return lax.all_to_all(
        produced.reshape(received.shape), "ep", split_axis=0, concat_axis=0, tiled=True
    )


def generic_device(
    stream, norm_gain, routing, gates, w_gate, w_up, w_down, shared_gate, shared_up, shared_down
):
    tok_rows, top_count = routing.shape
    local_count = w_gate.shape[0]
    peer_count = lax.axis_size("ep")
    experts = local_count * peer_count
    capacity = 2 * tok_rows * top_count // experts
    normed = layer_norm(stream, norm_gain)
    row_ids = jnp.arange(tok_rows, dtype=jnp.int32)
    lower = (row_ids[:, None] > row_ids[None, :]).astype(jnp.bfloat16)
    slot_ids = jnp.arange(capacity, dtype=jnp.int32).astype(jnp.float32)
    expert_hits = (
        routing[:, :, None] == jnp.arange(experts, dtype=jnp.int32)[None, None, :]
    ).astype(jnp.float32)
    token_hits = jnp.sum(expert_hits, axis=1).astype(jnp.bfloat16)
    earlier = jnp.dot(lower, token_hits, preferred_element_type=jnp.float32)
    slot_index = jnp.sum(earlier[:, None, :] * expert_hits, axis=2)
    slot_hits = (slot_index[:, :, None] == slot_ids[None, None, :]).astype(jnp.float32)
    gate_table = jnp.sum(
        gates[:, :, None, None] * expert_hits[:, :, :, None] * slot_hits[:, :, None, :], axis=1
    )
    all_normed = lax.all_gather(normed, "ep", axis=0, tiled=True)
    all_routing = lax.all_gather(routing, "ep", axis=0, tiled=True)
    first_expert = lax.axis_index("ep") * local_count
    shifted = all_routing.reshape(peer_count, tok_rows, top_count) - first_expert
    local_hits = (
        shifted[:, :, :, None] == jnp.arange(local_count, dtype=jnp.int32)[None, None, None, :]
    ).astype(jnp.float32)
    hits_here = jnp.sum(local_hits, axis=2).astype(jnp.bfloat16)
    prior_here = jnp.einsum("ab,pbx->pax", lower, hits_here, preferred_element_type=jnp.float32)
    placing_here = (
        hits_here.astype(jnp.float32)[:, :, :, None]
        * (prior_here[:, :, :, None] == slot_ids[None, None, None, :]).astype(jnp.float32)
    ).astype(jnp.bfloat16)
    sources = all_normed.reshape(peer_count, tok_rows, all_normed.shape[1])
    incoming = jnp.einsum(
        "ptxc,ptd->pxcd", placing_here, sources, preferred_element_type=jnp.float32
    ).astype(jnp.bfloat16)
    returned = serve_rows(
        incoming.reshape(peer_count * local_count, capacity, all_normed.shape[1]),
        w_gate,
        w_up,
        w_down,
    )
    weight_high = gate_table.astype(jnp.bfloat16)
    weight_low = (gate_table - weight_high.astype(jnp.float32)).astype(jnp.bfloat16)
    routed = jnp.einsum("tec,ecd->td", weight_high, returned, preferred_element_type=jnp.float32)
    routed = routed + jnp.einsum(
        "tec,ecd->td", weight_low, returned, preferred_element_type=jnp.float32
    )
    shared = shared_branch(normed, shared_gate, shared_up, shared_down)
    return (routed + shared).astype(jnp.bfloat16)


OWN, FAR_Y, UP, DOWN, UP_Y, DOWN_Y, OPP, OPP_Y = range(8)
KEYS = (
    ["A", "B", "D", "C0", "C1", "E", "F", "G"]
    + ["S%d" % s for s in range(8)]
    + ["mA", "mB", "mD", "mC", "mE", "mF", "mG"]
    + ["mS%d" % s for s in range(8)]
    + ["P%d" % s for s in range(8)]
    + ["g", "cA", "cB", "a0", "a1", "b0", "b1", "e", "f", "d"]
)


def fused_kernel(
    sizes, stream, gain, meta_in, wg_hbm, wu_hbm, wd_hbm, sg_hbm, su_hbm, sd_hbm, out,
    tok0, tok1, meta, pair_in, full_in, half_in, wg, wu, wd, inc, slot_gate, place, shared,
    send_sem, recv_sem, load_sem,
):
    n, local_count, capacity, top = sizes
    rows, width = stream.shape
    half = rows // 2
    me = lax.axis_index("ep")
    z, y, core = me // 4, (me // 2) % 2, me % 2
    depth = n // 4

    def at(zz, yy, cc):
        return lax.rem(zz, depth) * 4 + yy * 2 + cc

    z_up, z_down = at(z + 1, y, core), at(z + depth - 1, y, core)
    y_far, sibling = at(z, 1 - y, core), at(z, y, 1 - core)

    barrier = pltpu.get_barrier_semaphore()
    for peer in (z_up, z_down, y_far, sibling):
        pl.semaphore_signal(
            barrier, inc=1, device_id={"ep": peer}, device_id_type=pl.DeviceIdType.MESH
        )

    loads = [
        pltpu.make_async_copy(src, dst, load_sem.at[i])
        for i, (src, dst) in enumerate(
            [
                (sg_hbm, wg.at[1]), (su_hbm, wu.at[1]), (sd_hbm, wd.at[1]),
                (wg_hbm.at[0], wg.at[0]), (wu_hbm.at[0], wu.at[0]), (wd_hbm.at[0], wd.at[0]),
                (wg_hbm.at[1], wg.at[1]), (wu_hbm.at[1], wu.at[1]), (wd_hbm.at[1], wd.at[1]),
            ]
        )
    ]
    for load in loads[:6]:
        load.start()

    low, high = pl.ds(0, half), pl.ds(half, half)

    def own_part(s):
        return tok0.at[8 + s] if s < 4 else tok0.at[s]

    routes = {
        "B": (tok0.at[OWN], tok0.at[DOWN], z_up),
        "A": (tok0.at[OWN], tok0.at[UP], z_down),
        "D": (tok0.at[OWN], tok0.at[FAR_Y], y_far),
        "C0": (tok0.at[DOWN, low], tok0.at[OPP, low], z_up),
        "C1": (tok0.at[UP, high], tok0.at[OPP, high], z_down),
        "F": (tok0.at[FAR_Y], tok0.at[DOWN_Y], z_up),
        "E": (tok0.at[FAR_Y], tok0.at[UP_Y], z_down),
        "G": (tok0.at[OPP], tok0.at[OPP_Y], y_far),
        "mB": (meta.at[OWN, 0], meta.at[DOWN, 0], z_up),
        "mA": (meta.at[OWN, 0], meta.at[UP, 0], z_down),
        "mD": (meta.at[OWN, 0], meta.at[FAR_Y, 0], y_far),
        "mC": (meta.at[DOWN, 0], meta.at[OPP, 0], z_up),
        "mF": (meta.at[FAR_Y, 0], meta.at[DOWN_Y, 0], z_up),
        "mE": (meta.at[FAR_Y, 0], meta.at[UP_Y, 0], z_down),
        "mG": (meta.at[OPP, 0], meta.at[OPP_Y, 0], y_far),
        "g": (own_part(OPP_Y), full_in.at[0], y_far),
        "e": (own_part(UP_Y), full_in.at[1], z_up),
        "f": (own_part(DOWN_Y), full_in.at[2], z_down),
        "d": (own_part(FAR_Y), full_in.at[3], y_far),
        "cA": (own_part(OPP).at[high], half_in.at[0], z_up),
        "cB": (own_part(OPP).at[low], half_in.at[1], z_down),
        "a0": (own_part(UP).at[low], full_in.at[4, low], z_up),
        "a1": (own_part(UP).at[high], full_in.at[4, high], z_up),
        "b0": (own_part(DOWN).at[low], full_in.at[5, low], z_down),
        "b1": (own_part(DOWN).at[high], full_in.at[5, high], z_down),
    }
    for s in range(8):
        routes["S%d" % s] = (tok0.at[s], tok1.at[s], sibling)
        routes["mS%d" % s] = (meta.at[s, 0], meta.at[s, 1], sibling)
        routes["P%d" % s] = (tok1.at[s], pair_in.at[s], sibling)

    def copy_of(key):
        src, dst, peer = routes[key]
        i = KEYS.index(key)
        return pltpu.make_async_remote_copy(
            src_ref=src, dst_ref=dst, send_sem=send_sem.at[i], recv_sem=recv_sem.at[i],
            device_id={"ep": peer}, device_id_type=pl.DeviceIdType.MESH,
        )

    def send(*keys):
        for key in keys:
            copy_of(key).start()

    def arrived(*keys):
        for key in keys:
            copy_of(key).wait_recv()

    def sent(*keys):
        for key in keys:
            copy_of(key).wait_send()

    piece = 32

    def norm_rows(i, carry):
        span = pl.ds(pl.multiple_of(i * piece, piece), piece)
        wide = stream[span, :].astype(jnp.float32)
        mean = jnp.mean(wide, axis=-1, keepdims=True)
        centred = wide - mean
        var = jnp.mean(centred * centred, axis=-1, keepdims=True)
        tok0[OWN, span, :] = (centred * lax.rsqrt(var + 1e-05) * gain[...]).astype(jnp.bfloat16)
        return carry

    lax.fori_loop(0, rows // piece, norm_rows, 0)
    meta[OWN, 0] = meta_in[...]
    pl.semaphore_wait(barrier, 4)
    send("mB", "mA", "mD", "mS0", "B", "A", "D", "S0")

    def hidden_of(x, slot):
        gate = jnp.dot(x, wg[slot], preferred_element_type=jnp.float32)
        up = jnp.dot(x, wu[slot], preferred_element_type=jnp.float32)
        return jax.nn.silu(gate) * up

    cols = width // 4

    for load in loads[:3]:
        load.wait()
    hidden = hidden_of(tok0[OWN], 1).astype(jnp.bfloat16)
    for c in range(4):
        part = pl.ds(c * cols, cols)
        shared[:, part] = jnp.dot(hidden, wd[1, :, part], preferred_element_type=jnp.float32)
    for load in loads[6:]:
        load.start()

    first = (me * local_count).astype(jnp.float32)
    tri = (
        lax.broadcasted_iota(jnp.int32, (rows, rows), 0)
        < lax.broadcasted_iota(jnp.int32, (rows, rows), 1)
    ).astype(jnp.float32).astype(jnp.bfloat16)
    slots = local_count * capacity
    slot_row = lax.broadcasted_iota(jnp.int32, (slots, rows), 0).astype(jnp.float32)
    stack_row = lax.broadcasted_iota(jnp.int32, (8, rows), 0)

    def serve_group(base):
        stacked = jnp.zeros((8, rows), jnp.float32)
        gate_rows, hit_rows = [], []
        for k in range(4):
            m = meta[base + k // 2, k % 2]
            ids, weights = m[0:top], m[top:2 * top]
            for x in range(local_count):
                match = (ids == first + x).astype(jnp.float32)
                hit = jnp.sum(match, axis=0, keepdims=True)
                hit_rows.append(hit)
                gate_rows.append(jnp.sum(match * weights, axis=0, keepdims=True))
                stacked = jnp.where(stack_row == k * local_count + x, hit, stacked)
        prior = jnp.dot(stacked.astype(jnp.bfloat16), tri, preferred_element_type=jnp.float32)
        for k in range(4):
            j, r = k // 2, k % 2
            chosen = jnp.zeros((slots, rows), jnp.float32)
            weighted = jnp.zeros((slots, rows), jnp.float32)
            for x in range(local_count):
                q = k * local_count + x
                row = jnp.where(hit_rows[q] > 0, prior[q:q + 1] + x * capacity, -1.0)
                same = (slot_row == row).astype(jnp.float32)
                chosen = chosen + same
                weighted = weighted + same * gate_rows[q]
            slot_gate[k] = jnp.broadcast_to(jnp.sum(weighted, axis=1, keepdims=True), (slots, 128))
            place[k] = chosen.astype(jnp.bfloat16)
            source = tok0 if r == 0 else tok1
            for c in range(4):
                part = pl.ds(c * cols, cols)
                inc[k, :, part] = jnp.dot(
                    place[k], source[base + j, :, part], preferred_element_type=jnp.float32
                ).astype(jnp.bfloat16)
        for x in range(local_count):
            mine = pl.ds(x * capacity, capacity)
            taken = inc[:, mine, :].reshape(4 * capacity, width)
            scale = slot_gate[:, mine, :].reshape(4 * capacity, 128)[:, 0:1]
            act = (hidden_of(taken, x) * scale).astype(jnp.bfloat16)
            for c in range(4):
                part = pl.ds(c * cols, cols)
                made = jnp.dot(act, wd[x, :, part], preferred_element_type=jnp.float32)
                inc[:, mine, part] = made.astype(jnp.bfloat16).reshape(4, capacity, cols)

    def combine_group(base, g):
        for k in range(4):
            j, r = k // 2, k % 2
            for c in range(4):
                part = pl.ds(c * cols, cols)
                total = lax.dot_general(
                    place[k], inc[k, :, part], (((0,), (0,)), ((), ())),
                    preferred_element_type=jnp.float32,
                ).astype(jnp.bfloat16)
                if r == 0:
                    tok0[base + j + 8 * (1 - g // 2), :, part] = total
                else:
                    tok1[base + j, :, part] = total

    def add_into(dst, others, begin, count):
        def step(i, carry):
            span = pl.ds(pl.multiple_of(begin + i * piece, piece), piece)
            total = dst[span, :].astype(jnp.float32)
            for other, offset in others:
                there = pl.ds(pl.multiple_of(begin - offset + i * piece, piece), piece)
                total = total + other[there, :].astype(jnp.float32)
            dst[span, :] = total.astype(jnp.bfloat16)
            return carry

        lax.fori_loop(0, count // piece, step, 0)

    def group(g, carry):
        @pl.when(g == 0)
        def _():
            arrived("mB", "mA", "mD", "mS0")
            send("mC", "mF", "mE", "mS1", "mS2", "mS3")
            arrived("B")
            send("C0", "S3")
            arrived("A")
            send("C1", "S2")
            arrived("D")
            send("F", "E", "S1")
            arrived("mC")
            send("mG", "mS6")
            arrived("mE", "mF")
            send("mS4", "mS5")
            for load in loads[3:]:
                load.wait()
            arrived("S0", "S1", "mS1")

        @pl.when(g == 1)
        def _():
            arrived("S2", "S3", "mS2", "mS3")

        @pl.when(g == 2)
        def _():
            arrived("C0", "C1")
            send("G", "S6")
            arrived("E")
            send("S4")
            arrived("F")
            send("S5")
            arrived("S4", "S5", "mS4", "mS5")

        @pl.when(g == 3)
        def _():
            arrived("mG", "G")
            send("mS7", "S7")
            arrived("mS6", "S6", "mS7", "S7")

        base = 2 * g
        serve_group(base)

        @pl.when(g == 2)
        def _():
            sent("S4", "S5")

        @pl.when(g == 3)
        def _():
            sent("S6", "G", "S7")

        combine_group(base, g)

        @pl.when(g == 0)
        def _():
            send("P0", "P1")

        @pl.when(g == 1)
        def _():
            send("P2", "P3")

        @pl.when(g == 2)
        def _():
            send("P4", "P5")
            arrived("P4")
            add_into(own_part(UP_Y), [(pair_in.at[UP_Y], 0)], 0, rows)
            send("e")
            arrived("P5")
            add_into(own_part(DOWN_Y), [(pair_in.at[DOWN_Y], 0)], 0, rows)
            send("f")

        @pl.when(g == 3)
        def _():
            send("P7", "P6")

        return carry

    lax.fori_loop(0, 4, group, 0)
    arrived("P7")
    add_into(own_part(OPP_Y), [(pair_in.at[OPP_Y], 0)], 0, rows)
    send("g")
    arrived("P2", "P3")
    add_into(own_part(UP), [(pair_in.at[UP], 0)], 0, half)
    send("a0")
    add_into(own_part(DOWN), [(pair_in.at[DOWN], 0)], half, half)
    send("b1")
    arrived("P0", "P1", "P6", "e", "f")
    add_into(
        own_part(FAR_Y), [(pair_in.at[FAR_Y], 0), (full_in.at[1], 0), (full_in.at[2], 0)], 0, rows
    )
    send("d")
    arrived("g")
    add_into(own_part(OPP), [(pair_in.at[OPP], 0), (full_in.at[0], 0)], 0, rows)
    send("cA", "cB")
    arrived("cA")
    add_into(own_part(UP), [(pair_in.at[UP], 0), (half_in.at[0], half)], half, half)
    send("a1")
    arrived("cB")
    add_into(own_part(DOWN), [(pair_in.at[DOWN], 0), (half_in.at[1], 0)], 0, half)
    send("b0")
    arrived("a0", "b1", "d", "a1", "b0")

    def finish(i, carry):
        span = pl.ds(pl.multiple_of(i * piece, piece), piece)
        total = shared[span, :] + tok0[8 + OWN, span, :].astype(jnp.float32)
        for other in (pair_in.at[OWN], full_in.at[3], full_in.at[4], full_in.at[5]):
            total = total + other[span, :].astype(jnp.float32)
        out[span, :] = total.astype(jnp.bfloat16)
        return carry

    lax.fori_loop(0, rows // piece, finish, 0)
    waited = ("S4", "S5", "S6", "G", "S7")
    sent(*[key for key in KEYS if key not in waited])


def fused_device(
    stream, norm_gain, routing, gates, w_gate, w_up, w_down, shared_gate, shared_up, shared_down
):
    rows, width = stream.shape
    top = routing.shape[1]
    local_count, _, hidden = w_gate.shape
    n = lax.axis_size("ep")
    capacity = 2 * rows * top // (local_count * n)
    slots = local_count * capacity
    meta = jnp.concatenate([routing.astype(jnp.float32), gates], axis=1).T
    bf16, f32 = jnp.bfloat16, jnp.float32
    vmem, anywhere = pl.BlockSpec(memory_space=pltpu.VMEM), pl.BlockSpec(memory_space=pl.ANY)
    return pl.pallas_call(
        functools.partial(fused_kernel, (n, local_count, capacity, top)),
        out_shape=jax.ShapeDtypeStruct((rows, width), bf16),
        in_specs=[vmem] * 3 + [anywhere] * 6,
        out_specs=vmem,
        scratch_shapes=[
            pltpu.VMEM((12, rows, width), bf16),
            pltpu.VMEM((8, rows, width), bf16),
            pltpu.VMEM((8, 2, 2 * top, rows), f32),
            pltpu.VMEM((8, rows, width), bf16),
            pltpu.VMEM((6, rows, width), bf16),
            pltpu.VMEM((2, rows // 2, width), bf16),
            pltpu.VMEM((2, width, hidden), bf16),
            pltpu.VMEM((2, width, hidden), bf16),
            pltpu.VMEM((2, hidden, width), bf16),
            pltpu.VMEM((4, slots, width), bf16),
            pltpu.VMEM((4, slots, 128), f32),
            pltpu.VMEM((4, slots, rows), bf16),
            pltpu.VMEM((rows, width), f32),
            pltpu.SemaphoreType.DMA((len(KEYS),)),
            pltpu.SemaphoreType.DMA((len(KEYS),)),
            pltpu.SemaphoreType.DMA((9,)),
        ],
        compiler_params=pltpu.CompilerParams(
            collective_id=0, has_side_effects=True, vmem_limit_bytes=63 * 1024 * 1024
        ),
    )(stream, norm_gain.reshape(1, -1), meta, w_gate, w_up, w_down, shared_gate, shared_up, shared_down)


def on_device(stream, norm_gain, routing, gates, w_gate, *rest):
    ring = lax.axis_size("ep") // 4
    fits = ring == 4 and w_gate.shape[0] == 2 and rest[2].shape == w_gate.shape[1:]
    run = fused_device if fits else generic_device
    return run(stream, norm_gain, routing, gates, w_gate, *rest)


def solution(mesh):
    placed = (
        P(("grp", "ep"), None),
        P(),
        P(("grp", "ep"), None),
        P(("grp", "ep"), None),
        P("ep", None, None),
        P("ep", None, None),
        P("ep", None, None),
        P(),
        P(),
        P(),
    )
    return jax.shard_map(
        on_device, mesh=mesh, in_specs=placed, out_specs=P(("grp", "ep"), None), check_vma=False
    )
```

```python
import functools
import jax
import jax.numpy as jnp
from jax import lax
from jax.experimental import pallas as pl
from jax.experimental.pallas import tpu as pltpu
from jax.sharding import PartitionSpec as P


def layer_norm(stream, norm_gain):
    widened = stream.astype(jnp.float32)
    row_mean = jnp.mean(widened, axis=-1, keepdims=True)
    variance = jnp.mean(jnp.square(widened - row_mean), axis=-1, keepdims=True)
    return ((widened - row_mean) * lax.rsqrt(variance + 1e-05) * norm_gain).astype(jnp.bfloat16)


def shared_branch(normed, shared_gate, shared_up, shared_down):
    shared_hidden = (
        jax.nn.silu(jnp.dot(normed, shared_gate, preferred_element_type=jnp.float32))
        * jnp.dot(normed, shared_up, preferred_element_type=jnp.float32)
    ).astype(jnp.bfloat16)
    return jnp.dot(shared_hidden, shared_down, preferred_element_type=jnp.float32)


def serve_rows(received, w_gate, w_up, w_down):
    local_count = w_gate.shape[0]
    blocks = received.reshape((-1, local_count) + received.shape[1:])
    gate_act = jnp.einsum("sxcd,xdh->sxch", blocks, w_gate, preferred_element_type=jnp.float32)
    up_act = jnp.einsum("sxcd,xdh->sxch", blocks, w_up, preferred_element_type=jnp.float32)
    hidden = (jax.nn.silu(gate_act) * up_act).astype(jnp.bfloat16)
    produced = jnp.einsum(
        "sxch,xhd->sxcd", hidden, w_down, preferred_element_type=jnp.float32
    ).astype(jnp.bfloat16)
    return lax.all_to_all(
        produced.reshape(received.shape), "ep", split_axis=0, concat_axis=0, tiled=True
    )


def generic_device(
    stream, norm_gain, routing, gates, w_gate, w_up, w_down, shared_gate, shared_up, shared_down
):
    tok_rows, top_count = routing.shape
    local_count = w_gate.shape[0]
    peer_count = lax.axis_size("ep")
    experts = local_count * peer_count
    capacity = 2 * tok_rows * top_count // experts
    normed = layer_norm(stream, norm_gain)
    row_ids = jnp.arange(tok_rows, dtype=jnp.int32)
    lower = (row_ids[:, None] > row_ids[None, :]).astype(jnp.bfloat16)
    slot_ids = jnp.arange(capacity, dtype=jnp.int32).astype(jnp.float32)
    expert_hits = (
        routing[:, :, None] == jnp.arange(experts, dtype=jnp.int32)[None, None, :]
    ).astype(jnp.float32)
    token_hits = jnp.sum(expert_hits, axis=1).astype(jnp.bfloat16)
    earlier = jnp.dot(lower, token_hits, preferred_element_type=jnp.float32)
    slot_index = jnp.sum(earlier[:, None, :] * expert_hits, axis=2)
    slot_hits = (slot_index[:, :, None] == slot_ids[None, None, :]).astype(jnp.float32)
    gate_table = jnp.sum(
        gates[:, :, None, None] * expert_hits[:, :, :, None] * slot_hits[:, :, None, :], axis=1
    )
    all_normed = lax.all_gather(normed, "ep", axis=0, tiled=True)
    all_routing = lax.all_gather(routing, "ep", axis=0, tiled=True)
    first_expert = lax.axis_index("ep") * local_count
    shifted = all_routing.reshape(peer_count, tok_rows, top_count) - first_expert
    local_hits = (
        shifted[:, :, :, None] == jnp.arange(local_count, dtype=jnp.int32)[None, None, None, :]
    ).astype(jnp.float32)
    hits_here = jnp.sum(local_hits, axis=2).astype(jnp.bfloat16)
    prior_here = jnp.einsum("ab,pbx->pax", lower, hits_here, preferred_element_type=jnp.float32)
    placing_here = (
        hits_here.astype(jnp.float32)[:, :, :, None]
        * (prior_here[:, :, :, None] == slot_ids[None, None, None, :]).astype(jnp.float32)
    ).astype(jnp.bfloat16)
    sources = all_normed.reshape(peer_count, tok_rows, all_normed.shape[1])
    incoming = jnp.einsum(
        "ptxc,ptd->pxcd", placing_here, sources, preferred_element_type=jnp.float32
    ).astype(jnp.bfloat16)
    returned = serve_rows(
        incoming.reshape(peer_count * local_count, capacity, all_normed.shape[1]),
        w_gate,
        w_up,
        w_down,
    )
    weight_high = gate_table.astype(jnp.bfloat16)
    weight_low = (gate_table - weight_high.astype(jnp.float32)).astype(jnp.bfloat16)
    routed = jnp.einsum("tec,ecd->td", weight_high, returned, preferred_element_type=jnp.float32)
    routed = routed + jnp.einsum(
        "tec,ecd->td", weight_low, returned, preferred_element_type=jnp.float32
    )
    shared = shared_branch(normed, shared_gate, shared_up, shared_down)
    return (routed + shared).astype(jnp.bfloat16)


PLACE = {1: 0, 7: 1, 2: 2, 6: 3, 3: 4, 5: 5, 0: 6, 4: 7}
OWN = PLACE[0]
KEYS = (
    ["M4", "N4"]
    + [way + str(k) + part for way, first in (("M", 1), ("N", 5)) for k in range(first, first + 3)
       for part in ("l", "h")]
    + ["mM1", "mM2", "mM3", "mM4", "mN7", "mN6", "mN5"]
    + ["S%d" % k for k in range(8)]
    + ["mS%d" % k for k in range(8)]
    + ["P%d" % k for k in range(8)]
    + ["u4", "d4"]
    + [way + str(k) + part for way, first in (("u", 1), ("d", 5)) for k in range(first, first + 3)
       for part in ("l", "h")]
)


def fused_kernel(
    sizes, stream, gain, meta_in, wg_hbm, wu_hbm, wd_hbm, sg_hbm, su_hbm, sd_hbm, out,
    tok0, tok1, meta, pair_in, flow_in, wg, wu, wd, inc, slot_gate, place, shared,
    send_sem, recv_sem, load_sem,
):
    n, local_count, capacity, top = sizes
    rows, width = stream.shape
    half = rows // 2
    me = lax.axis_index("ep")
    depth = n // 4
    chips = 2 * depth
    z, y, core = me // 4, (me // 2) % 2, me % 2
    spot = z + y * (chips - 1 - 2 * z)

    def at(where, cc):
        where = lax.rem(where, chips)
        yy = where // depth
        zz = where + yy * (chips - 1 - 2 * where)
        return zz * 4 + yy * 2 + cc

    up, down, sibling = at(spot + 1, core), at(spot + chips - 1, core), at(spot, 1 - core)

    barrier = pltpu.get_barrier_semaphore()
    for peer in (up, down, sibling):
        pl.semaphore_signal(
            barrier, inc=1, device_id={"ep": peer}, device_id_type=pl.DeviceIdType.MESH
        )

    loads = [
        pltpu.make_async_copy(src, dst, load_sem.at[i])
        for i, (src, dst) in enumerate(
            [
                (sg_hbm, wg.at[1]), (su_hbm, wu.at[1]), (sd_hbm, wd.at[1]),
                (wg_hbm.at[0], wg.at[0]), (wu_hbm.at[0], wu.at[0]), (wd_hbm.at[0], wd.at[0]),
                (wg_hbm.at[1], wg.at[1]), (wu_hbm.at[1], wu.at[1]), (wd_hbm.at[1], wd.at[1]),
            ]
        )
    ]
    for load in loads[:6]:
        load.start()

    low, high = pl.ds(0, half), pl.ds(half, half)

    def tok(k):
        return tok0.at[PLACE[k]]

    def own_part(k):
        return tok0.at[PLACE[k] + (8 if PLACE[k] < 6 else 0)]

    routes = {
        "M4": (tok(3).at[low], tok(4).at[low], down),
        "N4": (tok(5).at[high], tok(4).at[high], up),
        "mM4": (meta.at[PLACE[3], 0], meta.at[PLACE[4], 0], down),
        "u4": (own_part(4).at[high], flow_in.at[3, high], up),
        "d4": (own_part(4).at[low], flow_in.at[4, low], down),
    }
    for k in (1, 2, 3):
        routes["mM%d" % k] = (meta.at[PLACE[k - 1], 0], meta.at[PLACE[k], 0], down)
        behind = (9 - k) % 8
        routes["mN%d" % (8 - k)] = (meta.at[PLACE[behind], 0], meta.at[PLACE[8 - k], 0], up)
        for name, rows_of in (("l", low), ("h", high)):
            routes["M%d%s" % (k, name)] = (tok(k - 1).at[rows_of], tok(k).at[rows_of], down)
            routes["N%d%s" % (8 - k, name)] = (tok(behind).at[rows_of], tok(8 - k).at[rows_of], up)
            routes["u%d%s" % (k, name)] = (
                own_part(k).at[rows_of], flow_in.at[k - 1, rows_of], up
            )
            routes["d%d%s" % (8 - k, name)] = (
                own_part(8 - k).at[rows_of], flow_in.at[8 - k, rows_of], down
            )
    for k in range(8):
        s = PLACE[k]
        routes["S%d" % k] = (tok0.at[s], tok1.at[s], sibling)
        routes["mS%d" % k] = (meta.at[s, 0], meta.at[s, 1], sibling)
        routes["P%d" % k] = (tok1.at[s], pair_in.at[s], sibling)

    def copy_of(key):
        src, dst, peer = routes[key]
        i = KEYS.index(key)
        return pltpu.make_async_remote_copy(
            src_ref=src, dst_ref=dst, send_sem=send_sem.at[i], recv_sem=recv_sem.at[i],
            device_id={"ep": peer}, device_id_type=pl.DeviceIdType.MESH,
        )

    def send(*keys):
        for key in keys:
            copy_of(key).start()

    def arrived(*keys):
        for key in keys:
            copy_of(key).wait_recv()

    def sent(*keys):
        for key in keys:
            copy_of(key).wait_send()

    piece = 32

    def norm_rows(i, carry):
        span = pl.ds(pl.multiple_of(i * piece, piece), piece)
        wide = stream[span, :].astype(jnp.float32)
        mean = jnp.mean(wide, axis=-1, keepdims=True)
        centred = wide - mean
        var = jnp.mean(centred * centred, axis=-1, keepdims=True)
        tok0[OWN, span, :] = (centred * lax.rsqrt(var + 1e-05) * gain[...]).astype(jnp.bfloat16)
        return carry

    lax.fori_loop(0, rows // piece, norm_rows, 0)
    meta[OWN, 0] = meta_in[...]
    pl.semaphore_wait(barrier, 3)
    send("mM1", "mN7", "mS0", "M1l", "N7h", "M1h", "N7l", "S0")

    def hidden_of(x, slot):
        gate = jnp.dot(x, wg[slot], preferred_element_type=jnp.float32)
        up = jnp.dot(x, wu[slot], preferred_element_type=jnp.float32)
        return jax.nn.silu(gate) * up

    cols = width // 4

    for load in loads[:3]:
        load.wait()
    hidden = hidden_of(tok0[OWN], 1).astype(jnp.bfloat16)
    for c in range(4):
        part = pl.ds(c * cols, cols)
        shared[:, part] = jnp.dot(hidden, wd[1, :, part], preferred_element_type=jnp.float32)
    for load in loads[6:]:
        load.start()

    first = (me * local_count).astype(jnp.float32)
    tri = (
        lax.broadcasted_iota(jnp.int32, (rows, rows), 0)
        < lax.broadcasted_iota(jnp.int32, (rows, rows), 1)
    ).astype(jnp.float32).astype(jnp.bfloat16)
    slots = local_count * capacity
    slot_row = lax.broadcasted_iota(jnp.int32, (slots, rows), 0).astype(jnp.float32)
    stack_row = lax.broadcasted_iota(jnp.int32, (8, rows), 0)

    def serve_group(base):
        stacked = jnp.zeros((8, rows), jnp.float32)
        gate_rows, hit_rows = [], []
        for k in range(4):
            m = meta[base + k // 2, k % 2]
            ids, weights = m[0:top], m[top:2 * top]
            for x in range(local_count):
                match = (ids == first + x).astype(jnp.float32)
                hit = jnp.sum(match, axis=0, keepdims=True)
                hit_rows.append(hit)
                gate_rows.append(jnp.sum(match * weights, axis=0, keepdims=True))
                stacked = jnp.where(stack_row == k * local_count + x, hit, stacked)
        prior = jnp.dot(stacked.astype(jnp.bfloat16), tri, preferred_element_type=jnp.float32)
        for k in range(4):
            j, r = k // 2, k % 2
            chosen = jnp.zeros((slots, rows), jnp.float32)
            weighted = jnp.zeros((slots, rows), jnp.float32)
            for x in range(local_count):
                q = k * local_count + x
                row = jnp.where(hit_rows[q] > 0, prior[q:q + 1] + x * capacity, -1.0)
                same = (slot_row == row).astype(jnp.float32)
                chosen = chosen + same
                weighted = weighted + same * gate_rows[q]
            slot_gate[k] = jnp.broadcast_to(jnp.sum(weighted, axis=1, keepdims=True), (slots, 128))
            place[k] = chosen.astype(jnp.bfloat16)
            source = tok0 if r == 0 else tok1
            for c in range(4):
                part = pl.ds(c * cols, cols)
                inc[k, :, part] = jnp.dot(
                    place[k], source[base + j, :, part], preferred_element_type=jnp.float32
                ).astype(jnp.bfloat16)
        for x in range(local_count):
            mine = pl.ds(x * capacity, capacity)
            taken = inc[:, mine, :].reshape(4 * capacity, width)
            scale = slot_gate[:, mine, :].reshape(4 * capacity, 128)[:, 0:1]
            act = (hidden_of(taken, x) * scale).astype(jnp.bfloat16)
            for c in range(4):
                part = pl.ds(c * cols, cols)
                made = jnp.dot(act, wd[x, :, part], preferred_element_type=jnp.float32)
                inc[:, mine, part] = made.astype(jnp.bfloat16).reshape(4, capacity, cols)

    def combine_group(base, g):
        for k in range(4):
            j, r = k // 2, k % 2
            for c in range(4):
                part = pl.ds(c * cols, cols)
                total = lax.dot_general(
                    place[k], inc[k, :, part], (((0,), (0,)), ((), ())),
                    preferred_element_type=jnp.float32,
                ).astype(jnp.bfloat16)
                if r == 0:
                    tok0[base + j + 8 * (1 - g // 3), :, part] = total
                else:
                    tok1[base + j, :, part] = total

    def add_into(dst, others, begin, count):
        def step(i, carry):
            span = pl.ds(pl.multiple_of(begin + i * piece, piece), piece)
            total = dst[span, :].astype(jnp.float32)
            for other, offset in others:
                there = pl.ds(pl.multiple_of(begin - offset + i * piece, piece), piece)
                total = total + other[there, :].astype(jnp.float32)
            dst[span, :] = total.astype(jnp.bfloat16)
            return carry

        lax.fori_loop(0, count // piece, step, 0)

    def pair(k):
        return (pair_in.at[PLACE[k]], 0)

    def group(g, carry):
        @pl.when(g == 0)
        def _():
            arrived("mM1", "mN7")
            send("mM2", "mN6", "mS1", "mS7")
            arrived("M1l")
            send("M2l")
            arrived("N7h")
            send("N6h")
            arrived("M1h")
            send("M2h")
            arrived("N7l")
            send("N6l", "S1", "S7")
            for load in loads[3:]:
                load.wait()
            arrived("S1", "S7", "mS1", "mS7")

        @pl.when(g == 1)
        def _():
            arrived("mM2", "mN6")
            send("mM3", "mN5", "mS2", "mS6")
            arrived("M2l")
            send("M3l")
            arrived("N6h")
            send("N5h")
            arrived("M2h")
            send("M3h")
            arrived("N6l")
            send("N5l", "S2", "S6")
            arrived("S2", "S6", "mS2", "mS6")

        @pl.when(g == 2)
        def _():
            arrived("mM3", "mN5")
            send("mM4", "mS3", "mS5")
            arrived("M3l")
            send("M4")
            arrived("N5h")
            send("N4")
            arrived("M3h", "N5l")
            send("S3", "S5")
            arrived("S3", "S5", "mS3", "mS5")

        @pl.when(g == 3)
        def _():
            arrived("mM4", "M4", "N4")
            send("mS4", "S4")
            arrived("S0", "mS0", "S4", "mS4")

        base = 2 * g
        serve_group(base)

        @pl.when(g == 3)
        def _():
            sent("S0", "S4", "M1l", "M1h", "N7l", "N7h")

        combine_group(base, g)

        @pl.when(g == 0)
        def _():
            send("P1", "P7")

        @pl.when(g == 1)
        def _():
            send("P2", "P6")

        @pl.when(g == 2)
        def _():
            send("P3", "P5")
            arrived("P3")
            add_into(own_part(3), [pair(3)], 0, half)
            send("u3l")
            arrived("P5")
            add_into(own_part(5), [pair(5)], half, half)
            send("d5h")

        @pl.when(g == 3)
        def _():
            send("P4", "P0")

        return carry

    lax.fori_loop(0, 4, group, 0)
    arrived("P4")
    add_into(own_part(4), [pair(4)], half, half)
    send("u4")
    add_into(own_part(4), [pair(4)], 0, half)
    send("d4")
    arrived("P0", "P1", "P2", "P6", "P7")

    def pass_on(key, dst, k, landing, begin):
        arrived(key)
        add_into(dst, [pair(k), (flow_in.at[landing], 0)], begin, half)

    pass_on("u4", own_part(3), 3, 3, half)
    send("u3h")
    pass_on("d4", own_part(5), 5, 4, 0)
    send("d5l")
    for k in (2, 1):
        for name, begin in (("l", 0), ("h", half)):
            other = "h" if name == "l" else "l"
            pass_on("u%d%s" % (k + 1, name), own_part(k), k, k, begin)
            send("u%d%s" % (k, name))
            pass_on("d%d%s" % (7 - k, other), own_part(8 - k), 8 - k, 7 - k, half - begin)
            send("d%d%s" % (8 - k, other))
    arrived("u1l", "u1h", "d7l", "d7h")

    def finish(i, carry):
        span = pl.ds(pl.multiple_of(i * piece, piece), piece)
        total = shared[span, :] + tok0[OWN, span, :].astype(jnp.float32)
        for other in (pair_in.at[OWN], flow_in.at[0], flow_in.at[7]):
            total = total + other[span, :].astype(jnp.float32)
        out[span, :] = total.astype(jnp.bfloat16)
        return carry

    lax.fori_loop(0, rows // piece, finish, 0)
    waited = ("S0", "S4", "M1l", "M1h", "N7l", "N7h")
    sent(*[key for key in KEYS if key not in waited])


def fused_device(
    stream, norm_gain, routing, gates, w_gate, w_up, w_down, shared_gate, shared_up, shared_down
):
    rows, width = stream.shape
    top = routing.shape[1]
    local_count, _, hidden = w_gate.shape
    n = lax.axis_size("ep")
    capacity = 2 * rows * top // (local_count * n)
    slots = local_count * capacity
    meta = jnp.concatenate([routing.astype(jnp.float32), gates], axis=1).T
    bf16, f32 = jnp.bfloat16, jnp.float32
    vmem, anywhere = pl.BlockSpec(memory_space=pltpu.VMEM), pl.BlockSpec(memory_space=pl.ANY)
    return pl.pallas_call(
        functools.partial(fused_kernel, (n, local_count, capacity, top)),
        out_shape=jax.ShapeDtypeStruct((rows, width), bf16),
        in_specs=[vmem] * 3 + [anywhere] * 6,
        out_specs=vmem,
        scratch_shapes=[
            pltpu.VMEM((14, rows, width), bf16),
            pltpu.VMEM((8, rows, width), bf16),
            pltpu.VMEM((8, 2, 2 * top, rows), f32),
            pltpu.VMEM((8, rows, width), bf16),
            pltpu.VMEM((8, rows, width), bf16),
            pltpu.VMEM((2, width, hidden), bf16),
            pltpu.VMEM((2, width, hidden), bf16),
            pltpu.VMEM((2, hidden, width), bf16),
            pltpu.VMEM((4, slots, width), bf16),
            pltpu.VMEM((4, slots, 128), f32),
            pltpu.VMEM((4, slots, rows), bf16),
            pltpu.VMEM((rows, width), f32),
            pltpu.SemaphoreType.DMA((len(KEYS),)),
            pltpu.SemaphoreType.DMA((len(KEYS),)),
            pltpu.SemaphoreType.DMA((9,)),
        ],
        compiler_params=pltpu.CompilerParams(
            collective_id=0, has_side_effects=True, vmem_limit_bytes=63 * 1024 * 1024
        ),
    )(stream, norm_gain.reshape(1, -1), meta, w_gate, w_up, w_down, shared_gate, shared_up, shared_down)


def on_device(stream, norm_gain, routing, gates, w_gate, *rest):
    ring = lax.axis_size("ep") // 4
    fits = ring == 4 and w_gate.shape[0] == 2 and rest[2].shape == w_gate.shape[1:]
    run = fused_device if fits else generic_device
    return run(stream, norm_gain, routing, gates, w_gate, *rest)


def solution(mesh):
    placed = (
        P(("grp", "ep"), None),
        P(),
        P(("grp", "ep"), None),
        P(("grp", "ep"), None),
        P("ep", None, None),
        P("ep", None, None),
        P("ep", None, None),
        P(),
        P(),
        P(),
    )
    return jax.shard_map(
        on_device, mesh=mesh, in_specs=placed, out_specs=P(("grp", "ep"), None), check_vma=False
    )
```
